32 devices in a mesh: ep: 8 (over z, y), tp: 4 (over x, core).
Axes of the slice: x: 2, y: 2, z: 4, core: 2. Of those that a mesh axis runs over, the one named last changes fastest.
Arguments:
- hidden: bfloat16 [256, 2048], P('ep')
- norm_gains: float32 [4, 2048], replicated, may hold values from 0.1 to 1.9
- w_query: bfloat16 [2048, 1024], P(None, 'tp'), may hold values from -0.125 to 0.125
- w_key: bfloat16 [2048, 1024], P(None, 'tp'), may hold values from -0.125 to 0.125
- w_value: bfloat16 [2048, 1024], P(None, 'tp'), may hold values from -0.125 to 0.125
- w_outgate: bfloat16 [2048, 1024], P(None, 'tp'), may hold values from -0.125 to 0.125
- w_input_gate: bfloat16 [2048, 8], replicated, may hold values from -0.125 to 0.125
- w_forget_gate: bfloat16 [2048, 8], replicated, may hold values from -0.125 to 0.125
- forget_bias: float32 [8], replicated, may hold values from -1 to 4
- w_mix_out: bfloat16 [1024, 2048], P('tp')
- state_matrix: float32 [256, 8, 128, 128], P('ep', 'tp'), may hold values from -0.6 to 0.6
- state_norm: float32 [256, 8, 128], P('ep', 'tp'), may hold values from -0.6 to 0.6
- state_max: float32 [256, 8], P('ep', 'tp'), may hold values from -4 to 4
- routes: int32 [256, 2], P('ep'), may hold values from 0 to 7, all different within a row; in each aligned block of 32 rows (0 to 31, 32 to 63, ...) at most 16 rows name the same one
- route_scores: float32 [256, 2], P('ep'), may hold values from 0.1 to 1
- expert_gate: bfloat16 [8, 2048, 3584], P('ep', None, 'tp'), may hold values from -0.125 to 0.125
- expert_up: bfloat16 [8, 2048, 3584], P('ep', None, 'tp'), may hold values from -0.125 to 0.125
- expert_down: bfloat16 [8, 3584, 2048], P('ep', 'tp')
- dense_gate: bfloat16 [2048, 5632], P('tp', 'ep'), may hold values from -0.125 to 0.125
- dense_up: bfloat16 [2048, 5632], P('tp', 'ep'), may hold values from -0.125 to 0.125
- dense_down: bfloat16 [5632, 2048], P('ep', 'tp')
- dense_mix: float32 [2048], replicated, may hold values from -0.25 to 0.25
Outputs:
- new_hidden: bfloat16 [256, 2048], P('ep', 'tp')
- new_matrix: float32 [256, 8, 128, 128], P('ep', 'tp')
- new_norm: float32 [256, 8, 128], P('ep', 'tp')
- new_max: float32 [256, 8], P('ep', 'tp')
The draws below stay inside these ranges and needn't reach their ends.
Inputs may be any that keep to these rules, and one draw needn't show every extreme that they name: `routes`: each row names 2 different experts. Among the rows of one index of ep (an aligned block of 32 rows) no expert is named by more than 16 rows, and in every draw some expert is named by exactly 16 rows of some block.
All inputs are finite; a program needn't handle non-finite values.
Results may differ from the reference program's by a relative error of at most 0.02.
Values may be sent and summed in bfloat16 or wider, within the bound.
A program may use at most 128 MiB of HBM per device.

```python
import math
import jax
import jax.numpy as jnp
import numpy as np
from jax import lax

D = 2048
HEADS = 8
HEAD = 128
FF_E = 3584
FF = 5632
TOP = 2
SEQ_DEV = 32
EXPERTS = 8
CAP = 16
SEQS = 256
N_EP = 8
N_TP = 4


def column_scaled(key, array_shape, fan_in, marker):
    noise_key, level_key = jax.random.split(jax.random.fold_in(key, marker))
    columns = array_shape[-1]
    position = jnp.arange(columns, dtype=jnp.float32) / columns
    levels = 0.5 * position + 0.5 * jax.random.uniform(level_key, (columns,), jnp.float32)
    noise = jax.random.normal(noise_key, array_shape, jnp.float32)
    scales = 10.0 ** levels
    scales = scales / jnp.sqrt(jnp.mean(scales * scales))
    return (noise * scales * (1.0 / fan_in) ** 0.5).astype(jnp.bfloat16)


def draw_hidden(key, part):
    return column_scaled(key, (SEQS, D), 1, 101)


def draw_w_mix_out(key, part):
    return column_scaled(key, (HEADS * HEAD, D), HEADS * HEAD, 102)


def draw_expert_down(key, part):
    return column_scaled(key, (EXPERTS, FF_E, D), FF_E, 103)


def draw_dense_down(key, part):
    return column_scaled(key, (FF, D), FF, 104)


def block_levels(rng, shape, cuts, low, top_value):
    gain = 1.0
    for axis_at, parts in cuts:
        heights = jax.random.uniform(jax.random.fold_in(jax.random.fold_in(rng, 6), axis_at), (parts,), jnp.float32, low / len(cuts), top_value / len(cuts))
        gain = gain * jnp.repeat(jnp.exp(heights), shape[axis_at] // parts).reshape((-1,) + (1,) * (len(shape) - 1 - axis_at))
    return gain


def deal_out(own_key, own, number, rows, amount, top, limit, lean):
    order = jax.random.permutation(own_key, amount)
    heavy_load, ordinary = load_shares(amount, rows * top, limit, lean, True), load_shares(amount, rows * top, limit, lean, False)
    places = jnp.arange(amount)

    def named(tallies, rotation):
        used = int((tallies > 0).sum())
        fixed = max(1, used // 4)
        passed = fixed + (places - fixed + rotation * (used - fixed)) % max(1, amount - fixed)
        return jnp.zeros((amount,), jnp.int32).at[order[jnp.where(places < fixed, places, passed)]].set(jnp.asarray(tallies, jnp.int32))

    tallies = jnp.where(number % 4 == 0, named(heavy_load, number // 4), named(ordinary, number - number // 4 - 1))
    mixed = jax.random.permutation(jax.random.fold_in(own, 3), amount)
    giver, sink = mixed[0:amount // 2 * 2:2], mixed[1:amount // 2 * 2:2]
    slack = jnp.minimum(tallies[giver] - 1, limit - tallies[sink]) // 2
    slack = jnp.where((giver == order[0]) | (sink == order[0]) | (tallies[sink] == 0), 0, jnp.maximum(slack, 0))
    passed = jax.random.randint(jax.random.fold_in(own, 4), (amount // 2,), 0, 1 << 20) % (slack + 1)
    tallies = tallies.at[giver].add(-passed).at[sink].add(passed)
    members = jnp.searchsorted(jnp.cumsum(tallies), jnp.arange(rows * top), side="right").astype(jnp.int32)
    table = members.reshape(top, rows).T
    table = table[jax.random.permutation(jax.random.fold_in(own, 1), rows)]
    rotation = jax.random.randint(jax.random.fold_in(own, 2), (rows, 1), 0, top)
    return jnp.take_along_axis(table, (jnp.arange(top)[None, :] + rotation) % top, axis=1)


def load_shares(number_of, total, most, lean, full):
    portions = [(1 << 20) // math.isqrt(standing ** lean) + 1 for standing in range(1, number_of + 1)]
    largest = most if full else min(most, max(-(-total // number_of), total * portions[0] // sum(portions)))
    least = 1 if total - largest >= number_of - 1 else 0
    counts, surplus = [largest] + [least] * (number_of - 1), total - largest - least * (number_of - 1)
    while surplus > 0:
        candidates = [i for i in range(1, number_of) if counts[i] < largest] or [i for i in range(1, number_of) if counts[i] < most]
        pool, left = sum([portions[i] for i in candidates]), surplus
        for i in candidates:
            extra = min(most - counts[i], max(1, left * portions[i] // pool), surplus)
            counts[i] = counts[i] + extra
            surplus = surplus - extra
    return np.array(counts)


def normal_values(rng, dims, deviation, reach, shards=(), held_as=jnp.bfloat16):
    values = jax.random.normal(rng, dims, jnp.float32) * deviation
    if len(shards) > 0:
        values = block_levels(rng, dims, shards, -0.22, 0.18) * values
    return jnp.clip(values, min=-reach, max=reach).astype(held_as)


def setup_inputs(seed: int = 0) -> dict:
    arg_keys = jax.random.split(jax.random.key(seed), 23)
    hidden = draw_hidden(jax.random.fold_in(arg_keys[22], 71), 0)
    norm_gains = jnp.clip(1.0 + 0.18 * jax.random.normal(arg_keys[1], (4, D), jnp.float32), 0.1, 1.9)
    w_query = normal_values(arg_keys[2], (D, HEADS * HEAD), D ** -0.5, 0.125, ((1, 4),))
    w_key = normal_values(arg_keys[3], (D, HEADS * HEAD), D ** -0.5, 0.125, ((1, 4),))
    w_value = normal_values(arg_keys[4], (D, HEADS * HEAD), D ** -0.5, 0.125, ((1, 4),))
    w_outgate = normal_values(arg_keys[5], (D, HEADS * HEAD), D ** -0.5, 0.125, ((1, 4),))
    w_input_gate = normal_values(arg_keys[6], (D, HEADS), D ** -0.5, 0.125)
    w_forget_gate = normal_values(arg_keys[7], (D, HEADS), D ** -0.5, 0.125)
    forget_bias = jnp.clip(jax.random.uniform(arg_keys[8], (HEADS,), jnp.float32, -1.0, 4.0), -1.0, 4.0)
    w_mix_out = draw_w_mix_out(jax.random.fold_in(arg_keys[22], 71), 0)
    state_matrix = normal_values(arg_keys[10], (SEQS, HEADS, HEAD, HEAD), 0.1, 0.6, ((0, 8), (1, 4)), jnp.float32)
    state_norm = normal_values(arg_keys[11], (SEQS, HEADS, HEAD), 0.1, 0.6, ((0, 8), (1, 4)), jnp.float32)
    state_max = normal_values(arg_keys[12], (SEQS, HEADS), 1.0, 4.0, ((0, 8), (1, 4)), jnp.float32)
    routes_keys = jax.random.split(jax.random.fold_in(arg_keys[13], 1), SEQS // SEQ_DEV)
    routes_turns = jax.random.permutation(jax.random.fold_in(arg_keys[13], 3), SEQS // SEQ_DEV)
    routes = jax.vmap(lambda own, number: deal_out(jax.random.fold_in(arg_keys[13], 2), own, number, SEQ_DEV, EXPERTS, TOP, CAP, 2))(routes_keys, routes_turns).reshape((SEQS, TOP))
    route_scores = jnp.clip(jnp.exp(math.log(1.0) - 2.3025851 * jax.random.uniform(arg_keys[14], (SEQS, TOP), jnp.float32) ** block_levels(arg_keys[14], (SEQS, TOP), ((0, 8),), -0.2, 0.2)), 0.1, 1.0)
    expert_gate = normal_values(arg_keys[15], (EXPERTS, D, FF_E), D ** -0.5, 0.125, ((0, 8), (2, 4)))
    expert_up = normal_values(arg_keys[16], (EXPERTS, D, FF_E), D ** -0.5, 0.125, ((0, 8), (2, 4)))
    expert_down = draw_expert_down(jax.random.fold_in(arg_keys[22], 71), 0)
    dense_gate = normal_values(arg_keys[18], (D, FF), D ** -0.5, 0.125, ((0, 4), (1, 8)))
    dense_up = normal_values(arg_keys[19], (D, FF), D ** -0.5, 0.125, ((0, 4), (1, 8)))
    dense_down = draw_dense_down(jax.random.fold_in(arg_keys[22], 71), 0)
    dense_mix = normal_values(arg_keys[21], (D,), (D // 4) ** -0.5, 0.25, (), jnp.float32)
    return dict(hidden=hidden, norm_gains=norm_gains, w_query=w_query, w_key=w_key, w_value=w_value, w_outgate=w_outgate, w_input_gate=w_input_gate, w_forget_gate=w_forget_gate, forget_bias=forget_bias, w_mix_out=w_mix_out, state_matrix=state_matrix, state_norm=state_norm, state_max=state_max, routes=routes, route_scores=route_scores, expert_gate=expert_gate, expert_up=expert_up, expert_down=expert_down, dense_gate=dense_gate, dense_up=dense_up, dense_down=dense_down, dense_mix=dense_mix)


EPS = 1e-06

def inverse_rms(values):
    return lax.rsqrt(lax.optimization_barrier(jnp.mean(values * values, axis=-1, keepdims=True)) + EPS)

def settle(values):
    return lax.optimization_barrier(values.astype(jnp.bfloat16)).astype(jnp.float32)

def grouped_product(activations, weights_in):
    row_count, inner_width = activations.shape
    group_width = inner_width // N_TP
    left_side = activations.astype(jnp.float32).reshape(row_count, N_TP, group_width)
    right_side = weights_in.astype(jnp.float32).reshape(N_TP, group_width, weights_in.shape[1])
    pieces = settle(jnp.einsum('rbf,bfd->brd', left_side, right_side))
    return lax.optimization_barrier(jnp.sum(pieces, axis=0)).astype(jnp.bfloat16)

def reference(hidden, norm_gains, w_query, w_key, w_value, w_outgate, w_input_gate, w_forget_gate, forget_bias, w_mix_out, state_matrix, state_norm, state_max, routes, route_scores, expert_gate, expert_up, expert_down, dense_gate, dense_up, dense_down, dense_mix):
    start_f = hidden.astype(jnp.float32)
    normed_in = (start_f * inverse_rms(start_f) * norm_gains[0]).astype(jnp.bfloat16)

    def project(weight):
        return settle(jnp.dot(normed_in, weight, preferred_element_type=jnp.float32))
    query = project(w_query).reshape(SEQS, HEADS, HEAD)
    keys = project(w_key).reshape(SEQS, HEADS, HEAD) * HEAD ** (-0.5)
    values = project(w_value).reshape(SEQS, HEADS, HEAD)
    out_gate = project(w_outgate)
    in_gate = jnp.dot(normed_in, w_input_gate, preferred_element_type=jnp.float32)
    log_forget = jax.nn.log_sigmoid(jnp.dot(normed_in, w_forget_gate, preferred_element_type=jnp.float32) + forget_bias)
    carried = log_forget + state_max
    new_max = jnp.maximum(carried, in_gate)
    keep = jnp.exp(carried - new_max)
    write = jnp.exp(in_gate - new_max)
    written = write[:, :, None] * keys
    new_matrix = keep[:, :, None, None] * state_matrix + written[:, :, :, None] * values[:, :, None, :]
    new_norm = keep[:, :, None] * state_norm + written
    numer = jnp.einsum('shd,shdv->shv', query, new_matrix)
    denom = jnp.einsum('shd,shd->sh', query, new_norm)
    read = numer / jnp.maximum(jnp.abs(denom), jnp.exp(-new_max))[:, :, None]
    mixed = (jax.nn.sigmoid(out_gate) * read.reshape(SEQS, HEADS * HEAD)).astype(jnp.bfloat16)
    branch = settle(grouped_product(mixed, w_mix_out))
    residual_f = start_f + norm_gains[1] * branch * inverse_rms(branch)
    residual = settle(residual_f)
    scale_two = inverse_rms(residual_f)
    normed = (residual_f * scale_two * norm_gains[2]).astype(jnp.bfloat16)
    mix_gate = jax.nn.sigmoid(scale_two[:, 0] * lax.optimization_barrier(jnp.sum(residual_f * norm_gains[2] * dense_mix, axis=-1)))
    dense_pre_gate = jnp.dot(normed, dense_gate, preferred_element_type=jnp.float32)
    dense_pre_up = jnp.dot(normed, dense_up, preferred_element_type=jnp.float32)
    dense_hidden = (jax.nn.silu(dense_pre_gate) * dense_pre_up).astype(jnp.bfloat16)
    dense_out = jnp.dot(dense_hidden, dense_down, preferred_element_type=jnp.float32)
    pairs = routes.reshape(N_EP, SEQ_DEV * TOP).astype(jnp.int32)
    picks = (pairs[:, :, None] == jnp.arange(EXPERTS, dtype=jnp.int32)[None, None, :]).astype(jnp.int32)
    ranks = (lax.optimization_barrier(jnp.sum(jnp.cumsum(picks, axis=1) * picks, axis=-1)) - 1).astype(jnp.int32)
    buffer_row = (jnp.arange(N_EP, dtype=jnp.int32)[:, None] * CAP + ranks).reshape(-1).astype(jnp.int32)
    flat_expert = pairs.reshape(-1)
    token_index = (jnp.arange(SEQS * TOP, dtype=jnp.int32) // TOP).astype(jnp.int32)
    expert_in = jnp.zeros((EXPERTS, N_EP * CAP, D), jnp.bfloat16).at[flat_expert, buffer_row].set(normed[token_index])

    def run_expert(operands):
        inputs, gate_weight, up_weight, down_weight = operands
        gate_pre = jnp.dot(inputs, gate_weight, preferred_element_type=jnp.float32)
        up_pre = jnp.dot(inputs, up_weight, preferred_element_type=jnp.float32)
        hidden_units = (jax.nn.silu(gate_pre) * up_pre).astype(jnp.bfloat16)
        return grouped_product(hidden_units, down_weight)
    expert_out = lax.map(run_expert, (expert_in, expert_gate, expert_up, expert_down))
    picked = settle(expert_out[flat_expert, buffer_row]).reshape(SEQS, TOP, D)
    share = route_scores / lax.optimization_barrier(jnp.sum(route_scores, axis=-1, keepdims=True))
    ffn = lax.optimization_barrier(jnp.sum(share[:, :, None] * picked, axis=1)) + mix_gate[:, None] * dense_out
    new_hidden = (residual + norm_gains[3] * ffn * inverse_rms(ffn)).astype(jnp.bfloat16)
    return (new_hidden, new_matrix, new_norm, new_max)
```

```python
import functools

import jax
import jax.numpy as jnp
from jax import lax
from jax.experimental import pallas as pl
from jax.experimental.pallas import tpu as pltpu
from jax.sharding import PartitionSpec as P

EPS = 1e-06


def settle(values):
    return lax.optimization_barrier(values.astype(jnp.bfloat16)).astype(jnp.float32)


MESH = pl.DeviceIdType.MESH


def tail_kernel(
    tp_count,
    ep_count,
    capacity,
    terms_ref,
    hidden_ref,
    gains_ref,
    mix_ref,
    codes_ref,
    combine_ref,
    share_ref,
    eg_hbm,
    eu_hbm,
    ed_hbm,
    dg_hbm,
    du_hbm,
    dd_hbm,
    out_ref,
    eg,
    eu,
    ed,
    dg,
    du,
    dd,
    br_recv,
    st_send,
    st_recv,
    fs_send,
    fs_recv,
    code_recv,
    rows_in,
    xin,
    pre_send,
    pre_recv,
    hid,
    down_send,
    down_recv,
    eo_send,
    eo_recv,
    sum_send,
    returned,
    w_sem,
    tp_send,
    tp_recv,
    ep_send,
    ep_recv,
):
    tp = lax.axis_index("tp")
    ep = lax.axis_index("ep")
    seqs, width = hidden_ref.shape
    part = width // tp_count
    rows_all = ep_count * seqs
    rows_tp = rows_all // tp_count
    first = pl.multiple_of(tp * part, part)
    f32, bf16 = jnp.float32, jnp.bfloat16

    loads = []
    for i, (src, dst) in enumerate(
        ((dg_hbm, dg), (du_hbm, du), (eg_hbm.at[0], eg), (eu_hbm.at[0], eu), (dd_hbm, dd), (ed_hbm.at[0], ed))
    ):
        load = pltpu.make_async_copy(src, dst, w_sem.at[i])
        load.start()
        loads.append(load)

    barrier = pltpu.get_barrier_semaphore()
    for d in range(1, tp_count):
        pl.semaphore_signal(
            barrier, inc=1, device_id={"tp": lax.rem(tp + d, tp_count)}, device_id_type=MESH
        )
    for d in range(1, ep_count):
        pl.semaphore_signal(
            barrier, inc=1, device_id={"ep": lax.rem(ep + d, ep_count)}, device_id_type=MESH
        )
    pl.semaphore_wait(barrier, tp_count - 1 + ep_count - 1)

    def tp_copies(phase, src_of, dst):
        made = []
        for d in range(1, tp_count):
            peer = lax.rem(tp + d, tp_count)
            copy = pltpu.make_async_remote_copy(
                src_ref=src_of(peer),
                dst_ref=dst,
                send_sem=tp_send.at[phase, d - 1],
                recv_sem=tp_recv.at[phase, d - 1],
                device_id={"tp": peer},
                device_id_type=MESH,
            )
            copy.start()
            made.append(copy)
        return made

    def ep_copies(phase, src_of, dst):
        made = []
        for d in range(1, ep_count):
            peer = lax.rem(ep + d, ep_count)
            copy = pltpu.make_async_remote_copy(
                src_ref=src_of(peer),
                dst_ref=dst,
                send_sem=ep_send.at[phase, d - 1],
                recv_sem=ep_recv.at[phase, d - 1],
                device_id={"ep": peer},
                device_id_type=MESH,
            )
            copy.start()
            made.append(copy)
        return made

    def arrive(copies):
        for copy in copies:
            copy.wait_recv()

    def left(copies):
        for copy in copies:
            copy.wait_send()

    def from_tp(d):
        return lax.rem(tp + tp_count - d, tp_count)

    def from_ep(d):
        return lax.rem(ep + ep_count - d, ep_count)

    def columns(peer):
        return pl.ds(pl.multiple_of(peer * part, part), part)

    branch_copies = tp_copies(0, lambda peer: terms_ref.at[:, columns(peer)], br_recv.at[tp])
    code_copies = ep_copies(0, lambda peer: codes_ref, code_recv.at[ep])
    start_part = hidden_ref[:, pl.ds(first, part)].astype(f32)
    gain_one = gains_ref[1:2, pl.ds(first, part)]
    gain_two = gains_ref[2:3, pl.ds(first, part)]
    gain_three = gains_ref[3:4, pl.ds(first, part)]
    mix_weight = gain_two * mix_ref[:, pl.ds(first, part)]
    start_sq = jnp.sum(start_part * start_part, axis=1, keepdims=True)
    start_dot = jnp.sum(start_part * mix_weight, axis=1, keepdims=True)
    branch = terms_ref[:, pl.ds(first, part)].astype(f32)
    arrive(branch_copies)
    for d in range(1, tp_count):
        branch = branch + br_recv[from_tp(d)].astype(f32)
    branch = branch.astype(bf16).astype(f32)
    lifted = gain_one * branch
    sums = (
        jnp.sum(branch * branch, axis=1, keepdims=True),
        start_sq,
        jnp.sum(start_part * lifted, axis=1, keepdims=True),
        jnp.sum(lifted * lifted, axis=1, keepdims=True),
        start_dot,
        jnp.sum(lifted * mix_weight, axis=1, keepdims=True),
    )
    lane = lax.broadcasted_iota(jnp.int32, (seqs, 128), 1)
    packed = jnp.zeros((seqs, 128), f32)
    for i, value in enumerate(sums):
        packed = packed + jnp.where(lane == i, value, 0.0)
    st_send[...] = packed
    stat_copies = tp_copies(1, lambda peer: st_send, st_recv.at[tp])
    arrive(stat_copies)
    for d in range(1, tp_count):
        packed = packed + st_recv[from_tp(d)]
    branch_sq, start_sq, cross_sum, lifted_sq, start_dot, lifted_dot = (
        packed[:, i : i + 1] for i in range(6)
    )
    branch_scale = lax.rsqrt(branch_sq / width + EPS)
    residual_f = start_part + lifted * branch_scale
    resid_sq = start_sq + 2.0 * branch_scale * cross_sum + branch_scale * branch_scale * lifted_sq
    gate_dot = start_dot + branch_scale * lifted_dot
    scale_two = lax.rsqrt(resid_sq / width + EPS)
    mix_gate = jax.nn.sigmoid(scale_two * gate_dot)
    residual = residual_f.astype(bf16).astype(f32)
    normed = (residual_f * scale_two * gain_two).astype(bf16)
    my_rows = pl.ds(pl.multiple_of(ep * seqs, seqs), seqs)
    rows_in[my_rows, :] = normed
    row_copies = ep_copies(1, lambda peer: rows_in.at[my_rows], rows_in.at[my_rows])

    arrive(code_copies)
    codes = codes_ref[...]
    for d in range(1, ep_count):
        codes = codes + code_recv[from_ep(d)]
    expert = lax.broadcasted_iota(jnp.int32, codes.shape, 0)
    mine = jnp.sum(jnp.where(expert == ep, codes, 0.0), axis=0, keepdims=True)
    slots = ep_count * capacity
    slot = lax.broadcasted_iota(jnp.int32, (slots, rows_all), 0)
    token = lax.broadcasted_iota(jnp.int32, (slots, rows_all), 1)
    wanted = (lax.rem(slot, capacity) + 1).astype(f32)
    placing = jnp.where(
        jnp.logical_and(slot // capacity == token // seqs, mine == wanted), 1.0, 0.0
    ).astype(bf16)

    arrive(row_copies)
    rows = rows_in[...]
    xin[tp] = jnp.dot(placing, rows, preferred_element_type=f32).astype(bf16)
    expert_copies = tp_copies(2, lambda peer: xin.at[tp], xin.at[tp])

    loads[0].wait()
    loads[1].wait()
    pre_send[0] = jnp.dot(rows, dg[...], preferred_element_type=f32).astype(bf16)
    pre_send[1] = jnp.dot(rows, du[...], preferred_element_type=f32).astype(bf16)

    def block_rows(peer):
        return pl.ds(pl.multiple_of(peer * rows_tp, rows_tp), rows_tp)

    pre_copies = tp_copies(3, lambda peer: pre_send.at[:, block_rows(peer)], pre_recv.at[tp])

    loads[2].wait()
    loads[3].wait()
    gate_pre = jnp.dot(xin[tp], eg[columns(tp), :], preferred_element_type=f32)
    up_pre = jnp.dot(xin[tp], eu[columns(tp), :], preferred_element_type=f32)
    for d in range(1, tp_count):
        expert_copies[d - 1].wait_recv()
        source = from_tp(d)
        block = xin[source]
        gate_pre = gate_pre + jnp.dot(block, eg[columns(source), :], preferred_element_type=f32)
        up_pre = up_pre + jnp.dot(block, eu[columns(source), :], preferred_element_type=f32)
    hidden_units = (jax.nn.silu(gate_pre) * up_pre).astype(bf16)

    arrive(pre_copies)
    pre = pre_send[:, block_rows(tp), :].astype(f32)
    for d in range(1, tp_count):
        pre = pre + pre_recv[from_tp(d)].astype(f32)
    hid[block_rows(tp), :] = (jax.nn.silu(pre[0]) * pre[1]).astype(bf16)
    hid_copies = tp_copies(4, lambda peer: hid.at[block_rows(tp)], hid.at[block_rows(tp)])

    loads[5].wait()
    for t in range(tp_count):
        eo_send[t] = jnp.dot(
            hidden_units, ed[:, t * part : (t + 1) * part], preferred_element_type=f32
        ).astype(bf16)
    eo_copies = tp_copies(5, lambda peer: eo_send.at[peer], eo_recv.at[tp])

    loads[4].wait()
    arrive(hid_copies)
    down_send[...] = jnp.dot(hid[...], dd[...], preferred_element_type=f32).astype(bf16)

    def seq_rows(peer):
        return pl.ds(pl.multiple_of(peer * seqs, seqs), seqs)

    down_copies = ep_copies(2, lambda peer: down_send.at[seq_rows(peer)], down_recv.at[ep])

    arrive(eo_copies)
    total = eo_send[tp].astype(f32)
    for d in range(1, tp_count):
        total = total + eo_recv[from_tp(d)].astype(f32)
    sum_send[...] = total.astype(bf16)

    def slot_rows(peer):
        return pl.ds(pl.multiple_of(peer * capacity, capacity), capacity)

    back_copies = ep_copies(3, lambda peer: sum_send.at[slot_rows(peer)], returned.at[slot_rows(ep)])
    returned[slot_rows(ep), :] = sum_send[slot_rows(ep), :]

    arrive(down_copies)
    dense_out = down_send[seq_rows(ep), :].astype(f32)
    for d in range(1, ep_count):
        dense_out = dense_out + down_recv[from_ep(d)].astype(f32)
    ffn = mix_gate * dense_out
    arrive(back_copies)
    picked = jnp.dot(combine_ref[...], returned[...], preferred_element_type=f32)
    for k in range(share_ref.shape[1]):
        ffn = ffn + share_ref[:, k : k + 1] * picked[k * seqs : (k + 1) * seqs]
    squares = jnp.where(lane == 0, jnp.sum(ffn * ffn, axis=1, keepdims=True), 0.0)
    fs_send[...] = squares
    final_copies = tp_copies(6, lambda peer: fs_send, fs_recv.at[tp])
    scaled = gain_three * ffn
    arrive(final_copies)
    for d in range(1, tp_count):
        squares = squares + fs_recv[from_tp(d)]
    out_ref[...] = (residual + scaled * lax.rsqrt(squares[:, 0:1] / width + EPS)).astype(bf16)
    for copies in (
        branch_copies,
        code_copies,
        stat_copies,
        row_copies,
        expert_copies,
        pre_copies,
        hid_copies,
        eo_copies,
        down_copies,
        back_copies,
        final_copies,
    ):
        left(copies)


def tail(
    terms, hidden, norm_gains, dense_mix, routes, route_scores, weights
):
    tp_count = lax.axis_size("tp")
    ep_count = lax.axis_size("ep")
    ep_place = lax.axis_index("ep")
    seqs, width = hidden.shape
    part = width // tp_count
    expert_gate, expert_up, expert_down, dense_gate, dense_up, dense_down = weights
    units = expert_gate.shape[2]
    dense_units = dense_gate.shape[1]
    top = routes.shape[1]
    experts = ep_count * expert_gate.shape[0]
    limit = 2 * seqs * top // ep_count
    capacity = -(-limit // 16) * 16
    rows_all = ep_count * seqs
    f32, bf16 = jnp.float32, jnp.bfloat16
    names = jnp.arange(experts, dtype=jnp.int32)
    hits = routes[:, :, None] == names[None, None, :]
    named = jnp.any(hits, axis=1)
    order = jnp.arange(seqs, dtype=jnp.int32)
    earlier = (order[None, :] < order[:, None])[:, :, None] & named[None, :, :]
    rank = jnp.sum(earlier.astype(jnp.int32), axis=1)
    code = jnp.where(named, rank + 1, 0).astype(f32)
    block = jnp.arange(ep_count, dtype=jnp.int32)[None, :, None] == ep_place
    codes = jnp.where(block, code.T[:, None, :], 0.0).reshape(experts, rows_all)
    place = jnp.arange(capacity, dtype=jnp.int32)
    combine = (
        (hits.transpose(1, 0, 2)[:, :, :, None] & (rank[None, :, :, None] == place))
        .astype(bf16)
        .reshape(top * seqs, experts * capacity)
    )
    share = route_scores / jnp.sum(route_scores, axis=-1, keepdims=True)
    vmem = pl.BlockSpec(memory_space=pltpu.VMEM)
    hbm = pl.BlockSpec(memory_space=pl.ANY)
    slots = ep_count * capacity
    return pl.pallas_call(
        functools.partial(tail_kernel, tp_count, ep_count, capacity),
        out_shape=jax.ShapeDtypeStruct((seqs, part), bf16),
        in_specs=[vmem] * 7 + [hbm] * 6,
        out_specs=vmem,
        scratch_shapes=[
            pltpu.VMEM((width, units), bf16),
            pltpu.VMEM((width, units), bf16),
            pltpu.VMEM((units, width), bf16),
            pltpu.VMEM(dense_gate.shape, bf16),
            pltpu.VMEM(dense_up.shape, bf16),
            pltpu.VMEM(dense_down.shape, bf16),
            pltpu.VMEM((tp_count, seqs, part), bf16),
            pltpu.VMEM((seqs, 128), f32),
            pltpu.VMEM((tp_count, seqs, 128), f32),
            pltpu.VMEM((seqs, 128), f32),
            pltpu.VMEM((tp_count, seqs, 128), f32),
            pltpu.VMEM((ep_count, experts, rows_all), f32),
            pltpu.VMEM((rows_all, part), bf16),
            pltpu.VMEM((tp_count, slots, part), bf16),
            pltpu.VMEM((2, rows_all, dense_units), bf16),
            pltpu.VMEM((tp_count, 2, rows_all // tp_count, dense_units), bf16),
            pltpu.VMEM((rows_all, dense_units), bf16),
            pltpu.VMEM((rows_all, part), bf16),
            pltpu.VMEM((ep_count, seqs, part), bf16),
            pltpu.VMEM((tp_count, slots, part), bf16),
            pltpu.VMEM((tp_count, slots, part), bf16),
            pltpu.VMEM((slots, part), bf16),
            pltpu.VMEM((slots, part), bf16),
            pltpu.SemaphoreType.DMA((6,)),
            pltpu.SemaphoreType.DMA((7, tp_count - 1)),
            pltpu.SemaphoreType.DMA((7, tp_count - 1)),
            pltpu.SemaphoreType.DMA((4, ep_count - 1)),
            pltpu.SemaphoreType.DMA((4, ep_count - 1)),
        ],
        compiler_params=pltpu.CompilerParams(
            collective_id=0, has_side_effects=True, vmem_limit_bytes=56 * 1024 * 1024
        ),
        name="tail",
    )(
        terms,
        hidden,
        norm_gains,
        dense_mix.reshape(1, width),
        codes,
        combine,
        share,
        *weights,
    )


def local(
    hidden,
    norm_gains,
    w_query,
    w_key,
    w_value,
    w_outgate,
    w_input_gate,
    w_forget_gate,
    forget_bias,
    w_mix_out,
    state_matrix,
    state_norm,
    state_max,
    routes,
    route_scores,
    expert_gate,
    expert_up,
    expert_down,
    dense_gate,
    dense_up,
    dense_down,
    dense_mix,
):
    tp_place = lax.axis_index("tp")
    seq_local, width = hidden.shape
    heads_local = state_matrix.shape[1]
    head_width = state_matrix.shape[2]
    start_f = hidden.astype(jnp.float32)
    normed_in = (
        start_f
        * lax.rsqrt(jnp.mean(start_f * start_f, axis=-1, keepdims=True) + EPS)
        * norm_gains[0]
    ).astype(jnp.bfloat16)
    query_f = jnp.dot(normed_in, w_query, preferred_element_type=jnp.float32)
    key_f = jnp.dot(normed_in, w_key, preferred_element_type=jnp.float32)
    value_f = jnp.dot(normed_in, w_value, preferred_element_type=jnp.float32)
    gate_f = jnp.dot(normed_in, w_outgate, preferred_element_type=jnp.float32)
    head_first = tp_place * heads_local
    input_weight = lax.dynamic_slice_in_dim(w_input_gate, head_first, heads_local, 1)
    forget_weight = lax.dynamic_slice_in_dim(w_forget_gate, head_first, heads_local, 1)
    forget_local = lax.dynamic_slice_in_dim(forget_bias, head_first, heads_local, 0)
    in_gate = jnp.dot(normed_in, input_weight, preferred_element_type=jnp.float32)
    log_forget = jax.nn.log_sigmoid(
        jnp.dot(normed_in, forget_weight, preferred_element_type=jnp.float32) + forget_local
    )
    query = settle(query_f).reshape(seq_local, heads_local, head_width)
    keys = settle(key_f).reshape(seq_local, heads_local, head_width) * head_width ** (-0.5)
    values = settle(value_f).reshape(seq_local, heads_local, head_width)
    carried = log_forget + state_max
    new_max = jnp.maximum(carried, in_gate)
    keep = jnp.exp(carried - new_max)
    write = jnp.exp(in_gate - new_max)
    written = write[:, :, None] * keys
    new_matrix = (
        keep[:, :, None, None] * state_matrix + written[:, :, :, None] * values[:, :, None, :]
    )
    new_norm = keep[:, :, None] * state_norm + written
    numer = jnp.einsum("shd,shdv->shv", query, new_matrix)
    denom = jnp.einsum("shd,shd->sh", query, new_norm)
    read = numer / jnp.maximum(jnp.abs(denom), jnp.exp(-new_max))[:, :, None]
    mixed = (
        jax.nn.sigmoid(settle(gate_f)) * read.reshape(seq_local, heads_local * head_width)
    ).astype(jnp.bfloat16)
    terms = jnp.dot(mixed, w_mix_out, preferred_element_type=jnp.float32).astype(jnp.bfloat16)
    new_hidden = tail(
        terms,
        hidden,
        norm_gains,
        dense_mix,
        routes,
        route_scores,
        (expert_gate, expert_up, expert_down, dense_gate, dense_up, dense_down),
    )
    return (new_hidden, new_matrix, new_norm, new_max)


def solution(mesh):
    placed = (
        P("ep", None),
        P(),
        P(None, "tp"),
        P(None, "tp"),
        P(None, "tp"),
        P(None, "tp"),
        P(),
        P(),
        P(),
        P("tp", None),
        P("ep", "tp", None, None),
        P("ep", "tp", None),
        P("ep", "tp"),
        P("ep", None),
        P("ep", None),
        P("ep", None, "tp"),
        P("ep", None, "tp"),
        P("ep", "tp", None),
        P("tp", "ep"),
        P("tp", "ep"),
        P("ep", "tp"),
        P(),
    )
    return jax.shard_map(
        local,
        mesh=mesh,
        in_specs=placed,
        out_specs=(P("ep", "tp"), P("ep", "tp", None, None), P("ep", "tp", None), P("ep", "tp")),
        check_vma=False,
    )
```

```python
import functools

import jax
import jax.numpy as jnp
from jax import lax
from jax.experimental import pallas as pl
from jax.experimental.pallas import tpu as pltpu
from jax.sharding import PartitionSpec as P

EPS = 1e-06


def front_kernel(
    hidden_ref,
    gains_ref,
    in_ref,
    forget_ref,
    bias_ref,
    norm_ref,
    max_ref,
    wq_hbm,
    wk_hbm,
    wv_hbm,
    wo_hbm,
    wm_hbm,
    state_hbm,
    terms_ref,
    matrix_hbm,
    new_norm_ref,
    new_max_ref,
    wq,
    wk,
    wv,
    wo,
    wm,
    state,
    numer,
    w_sem,
    in_sem,
    out_sem,
):
    tp = lax.axis_index("tp")
    f32, bf16 = jnp.float32, jnp.bfloat16
    seqs = hidden_ref.shape[0]
    heads, head = state.shape[1], state.shape[2]
    chunks = in_sem.shape[0]
    step = seqs // chunks
    loads = []
    for i, (src, dst) in enumerate(((wk_hbm, wk), (wq_hbm, wq), (wv_hbm, wv), (wo_hbm, wo))):
        loads.append(pltpu.make_async_copy(src, dst, w_sem.at[i]))
        loads[i].start()
    fetches = []
    for c in range(chunks):
        rows = pl.ds(c * step, step)
        fetches.append(pltpu.make_async_copy(state_hbm.at[rows], state.at[rows], in_sem.at[c]))
        fetches[c].start()
    loads.append(pltpu.make_async_copy(wm_hbm, wm, w_sem.at[4]))
    loads[4].start()

    start = hidden_ref[...].astype(f32)
    scale = lax.rsqrt(jnp.mean(start * start, axis=1, keepdims=True) + EPS)
    normed = (start * scale * gains_ref[0:1, :]).astype(bf16)
    last = (((1,), (1,)), ((), ()))
    in_all = lax.dot_general(normed, in_ref[...], last, preferred_element_type=f32)
    forget_all = lax.dot_general(normed, forget_ref[...], last, preferred_element_type=f32)
    forget_all = forget_all + bias_ref[...]
    forget_all = jnp.minimum(forget_all, 0.0) - jnp.log(1.0 + jnp.exp(-jnp.abs(forget_all)))
    column = lax.broadcasted_iota(jnp.int32, in_all.shape, 1)
    here = lax.broadcasted_iota(jnp.int32, (seqs, seqs), 0)
    there = lax.broadcasted_iota(jnp.int32, (seqs, seqs), 1)
    projected = []
    for i, weight in enumerate((wk, wq, wv)):
        loads[i].wait()
        product = jnp.dot(normed, weight[...], preferred_element_type=f32)
        projected.append(product.astype(bf16).astype(f32))
    keys, query, values = projected
    pieces = []
    for h in range(heads):
        span = slice(h * head, (h + 1) * head)
        pieces.extend((keys[:, span], query[:, span]))
    turned = jnp.concatenate(pieces, axis=0).T
    keeps = []
    adds = []
    bounds = []
    for h in range(heads):
        span = slice(h * head, (h + 1) * head)
        mine = column == tp * heads + h
        in_gate = jnp.sum(jnp.where(mine, in_all, 0.0), axis=1, keepdims=True)
        log_forget = jnp.sum(jnp.where(mine, forget_all, 0.0), axis=1, keepdims=True)
        before = jnp.sum(jnp.where(here == there, max_ref[h : h + 1, :], 0.0), axis=1, keepdims=True)
        carried = log_forget + before
        new_max = jnp.maximum(carried, in_gate)
        keep = jnp.exp(carried - new_max)
        write = jnp.exp(in_gate - new_max) * head ** (-0.5)
        new_max_ref[h : h + 1, :] = jnp.sum(
            jnp.where(here == there, new_max, 0.0), axis=0, keepdims=True
        )
        new_norm = keep * norm_ref[:, h, :] + write * keys[:, span]
        new_norm_ref[:, h, :] = new_norm
        denom = jnp.sum(query[:, span] * new_norm, axis=1, keepdims=True)
        bounds.append(jnp.maximum(jnp.abs(denom), jnp.exp(-new_max)))
        keeps.append(jnp.broadcast_to(keep, (seqs, head)))
        adds.append(write * values[:, span])
    stores = []
    for c in range(chunks):
        fetches[c].wait()
        for s in range(c * step, (c + 1) * step):
            for h in range(heads):
                at = 2 * h * seqs + s
                key_col = turned[:, at : at + 1]
                query_col = turned[:, at + seqs : at + seqs + 1]
                new = keeps[h][s : s + 1, :] * state[s, h] + key_col * adds[h][s : s + 1, :]
                state[s, h] = new
                numer[h, s : s + 1, :] = jnp.sum(query_col * new, axis=0, keepdims=True)
        rows = pl.ds(c * step, step)
        stores.append(pltpu.make_async_copy(state.at[rows], matrix_hbm.at[rows], out_sem.at[c]))
        stores[c].start()
    loads[3].wait()
    gate = jnp.dot(normed, wo[...], preferred_element_type=f32).astype(bf16).astype(f32)
    mixed = []
    for h in range(heads):
        span = slice(h * head, (h + 1) * head)
        mixed.append((jax.nn.sigmoid(gate[:, span]) * (numer[h] / bounds[h])).astype(bf16))
    mixed = jnp.concatenate(mixed, axis=1)
    loads[4].wait()
    part = terms_ref.shape[2]
    for t in range(terms_ref.shape[0]):
        terms_ref[t] = jnp.dot(
            mixed, wm[:, t * part : (t + 1) * part], preferred_element_type=f32
        ).astype(bf16)
    for store in stores:
        store.wait()


def front(hidden, norm_gains, gate_weights, forget_bias, state_norm, state_max, weights, state_matrix):
    tp_count = lax.axis_size("tp")
    seqs, width = hidden.shape
    heads, head = state_matrix.shape[1], state_matrix.shape[2]
    f32, bf16 = jnp.float32, jnp.bfloat16
    chunks = 4
    vmem = pl.BlockSpec(memory_space=pltpu.VMEM)
    hbm = pl.BlockSpec(memory_space=pl.ANY)
    terms, matrix, norm, top = pl.pallas_call(
        front_kernel,
        out_shape=(
            jax.ShapeDtypeStruct((tp_count, seqs, width // tp_count), bf16),
            jax.ShapeDtypeStruct(state_matrix.shape, f32),
            jax.ShapeDtypeStruct(state_norm.shape, f32),
            jax.ShapeDtypeStruct((heads, seqs), f32),
        ),
        in_specs=[vmem] * 7 + [hbm] * 6,
        out_specs=(vmem, hbm, vmem, vmem),
        scratch_shapes=[pltpu.VMEM(weight.shape, bf16) for weight in weights]
        + [
            pltpu.VMEM(state_matrix.shape, f32),
            pltpu.VMEM((heads, seqs, head), f32),
            pltpu.SemaphoreType.DMA((5,)),
            pltpu.SemaphoreType.DMA((chunks,)),
            pltpu.SemaphoreType.DMA((chunks,)),
        ],
        compiler_params=pltpu.CompilerParams(vmem_limit_bytes=40 * 1024 * 1024),
        name="front",
    )(
        hidden,
        norm_gains,
        gate_weights[0].T,
        gate_weights[1].T,
        forget_bias.reshape(1, -1),
        state_norm,
        state_max.T,
        *weights,
        state_matrix,
    )
    return terms, matrix, norm, top.T


MESH = pl.DeviceIdType.MESH


def tail_kernel(
    tp_count,
    ep_count,
    capacity,
    terms_ref,
    hidden_ref,
    gains_ref,
    mix_ref,
    routes_ref,
    scores_ref,
    eg_hbm,
    eu_hbm,
    ed_hbm,
    dg_hbm,
    du_hbm,
    dd_hbm,
    out_ref,
    eg,
    eu,
    ed,
    dg,
    du,
    dd,
    br_recv,
    st_send,
    st_recv,
    fs_send,
    fs_recv,
    code_send,
    code_recv,
    rows_in,
    xin,
    pre_send,
    pre_one,
    pre_mid,
    pre_two,
    hid,
    down_send,
    down_recv,
    eo_send,
    eo_one,
    eo_mid,
    eo_two,
    sum_send,
    returned,
    w_sem,
    tp_send,
    tp_recv,
    ep_send,
    ep_recv,
):
    tp = lax.axis_index("tp")
    ep = lax.axis_index("ep")
    seqs, width = hidden_ref.shape
    part = width // tp_count
    rows_all = ep_count * seqs
    rows_tp = rows_all // tp_count
    first = pl.multiple_of(tp * part, part)
    f32, bf16 = jnp.float32, jnp.bfloat16

    loads = []
    for i, (src, dst) in enumerate(
        ((dg_hbm, dg), (du_hbm, du), (eg_hbm.at[0], eg), (eu_hbm.at[0], eu), (dd_hbm, dd), (ed_hbm.at[0], ed))
    ):
        load = pltpu.make_async_copy(src, dst, w_sem.at[i])
        load.start()
        loads.append(load)

    barrier = pltpu.get_barrier_semaphore()
    for d in range(1, tp_count):
        pl.semaphore_signal(
            barrier, inc=1, device_id={"tp": lax.rem(tp + d, tp_count)}, device_id_type=MESH
        )
    for d in range(1, ep_count):
        pl.semaphore_signal(
            barrier, inc=1, device_id={"ep": lax.rem(ep + d, ep_count)}, device_id_type=MESH
        )
    pl.semaphore_wait(barrier, tp_count - 1 + ep_count - 1)

    def tp_copies(phase, src_of, dst):
        made = []
        for d in range(1, tp_count):
            peer = lax.rem(tp + d, tp_count)
            copy = pltpu.make_async_remote_copy(
                src_ref=src_of(peer),
                dst_ref=dst,
                send_sem=tp_send.at[phase, d - 1],
                recv_sem=tp_recv.at[phase, d - 1],
                device_id={"tp": peer},
                device_id_type=MESH,
            )
            copy.start()
            made.append(copy)
        return made

    groups = tp_count // 2
    parity = lax.rem(tp, 2)
    group = tp // 2
    pair = tp + 1 - 2 * parity

    def one_copy(phase, i, src, dst, peer):
        copy = pltpu.make_async_remote_copy(
            src_ref=src,
            dst_ref=dst,
            send_sem=tp_send.at[phase, i],
            recv_sem=tp_recv.at[phase, i],
            device_id={"tp": peer},
            device_id_type=MESH,
        )
        copy.start()
        return copy

    def ahead(d):
        return lax.rem(group + d, groups) * 2 + parity

    def behind(d):
        return lax.rem(group + groups - d, groups) * 2 + parity

    def gather_start(phase, at):
        made = [one_copy(phase, d - 1, at(tp), at(tp), ahead(d)) for d in range(1, groups)]
        made.append(one_copy(phase, groups - 1, at(tp), at(tp), pair))
        return made

    def gather_relay(phase, at, made):
        for d in range(1, groups):
            made[d - 1].wait_recv()
            made.append(one_copy(phase, groups - 1 + d, at(behind(d)), at(behind(d)), pair))

    def scatter_pair(phase, at, one):
        return [
            one_copy(phase, j, at(j * 2 + 1 - parity), one.at[j], pair) for j in range(groups)
        ]

    def scatter_cross(phase, at, one, mid, two, made):
        arrive(made)
        for d in range(1, groups):
            j = lax.rem(group + d, groups)
            mid[j] = (at(ahead(d))[...].astype(f32) + one[j].astype(f32)).astype(bf16)
            made.append(one_copy(phase, groups + d - 1, mid.at[j], two.at[group], ahead(d)))

    def scatter_sum(at, one, two, made):
        total = at(tp)[...].astype(f32) + one[group].astype(f32)
        for d in range(1, groups):
            made[groups + d - 1].wait_recv()
            total = total + two[lax.rem(group + groups - d, groups)].astype(f32)
        return total

    def ep_copies(phase, src_of, dst):
        made = []
        for d in range(1, ep_count):
            peer = lax.rem(ep + d, ep_count)
            copy = pltpu.make_async_remote_copy(
                src_ref=src_of(peer),
                dst_ref=dst,
                send_sem=ep_send.at[phase, d - 1],
                recv_sem=ep_recv.at[phase, d - 1],
                device_id={"ep": peer},
                device_id_type=MESH,
            )
            copy.start()
            made.append(copy)
        return made

    def arrive(copies):
        for copy in copies:
            copy.wait_recv()

    def left(copies):
        for copy in copies:
            copy.wait_send()

    def from_tp(d):
        return lax.rem(tp + tp_count - d, tp_count)

    def from_ep(d):
        return lax.rem(ep + ep_count - d, ep_count)

    def columns(peer):
        return pl.ds(pl.multiple_of(peer * part, part), part)

    branch_copies = tp_copies(0, lambda peer: terms_ref.at[peer], br_recv.at[tp])
    top = routes_ref.shape[0]
    experts = code_send.shape[0]
    name = lax.broadcasted_iota(jnp.int32, (experts, seqs), 0)
    hits = [routes_ref[k : k + 1, :] == name for k in range(top)]
    named = hits[0]
    for k in range(1, top):
        named = jnp.logical_or(named, hits[k])
    named = jnp.where(named, 1.0, 0.0)
    here = lax.broadcasted_iota(jnp.int32, (seqs, seqs), 0)
    there = lax.broadcasted_iota(jnp.int32, (seqs, seqs), 1)
    before = jnp.where(here < there, 1.0, 0.0).astype(bf16)
    rank = jnp.dot(named.astype(bf16), before, preferred_element_type=f32) + 1.0
    code = (named * rank).astype(bf16)
    from_row = lax.broadcasted_iota(jnp.int32, (seqs, rows_all), 0)
    to_row = lax.broadcasted_iota(jnp.int32, (seqs, rows_all), 1)
    spread = jnp.where(from_row + ep * seqs == to_row, 1.0, 0.0).astype(bf16)
    code_send[...] = jnp.dot(code, spread, preferred_element_type=f32)
    code_copies = ep_copies(0, lambda peer: code_send, code_recv.at[ep])
    slots = ep_count * capacity
    owner = lax.broadcasted_iota(jnp.int32, (slots, experts), 0) // capacity
    of_expert = lax.broadcasted_iota(jnp.int32, (slots, experts), 1)
    widen = jnp.where(owner == of_expert, 1.0, 0.0).astype(bf16)
    row_slot = lax.broadcasted_iota(jnp.int32, (slots, seqs), 0)
    row_wanted = (lax.rem(row_slot, capacity) + 1).astype(f32)
    combines = []
    shares = []
    score_sum = scores_ref[0:1, :]
    for k in range(1, top):
        score_sum = score_sum + scores_ref[k : k + 1, :]
    for k in range(top):
        code_k = jnp.where(hits[k], rank, 0.0).astype(bf16)
        wide = jnp.dot(widen, code_k, preferred_element_type=f32)
        combines.append(jnp.where(wide == row_wanted, 1.0, 0.0).astype(bf16))
        share = scores_ref[k : k + 1, :] / score_sum
        shares.append(jnp.sum(jnp.where(here == there, share, 0.0), axis=1, keepdims=True))
    start_part = hidden_ref[:, pl.ds(first, part)].astype(f32)
    gain_one = gains_ref[1:2, pl.ds(first, part)]
    gain_two = gains_ref[2:3, pl.ds(first, part)]
    gain_three = gains_ref[3:4, pl.ds(first, part)]
    mix_weight = gain_two * mix_ref[:, pl.ds(first, part)]
    start_sq = jnp.sum(start_part * start_part, axis=1, keepdims=True)
    start_dot = jnp.sum(start_part * mix_weight, axis=1, keepdims=True)
    branch = terms_ref[tp].astype(f32)
    arrive(branch_copies)
    for d in range(1, tp_count):
        branch = branch + br_recv[from_tp(d)].astype(f32)
    branch = branch.astype(bf16).astype(f32)
    lifted = gain_one * branch
    sums = (
        jnp.sum(branch * branch, axis=1, keepdims=True),
        start_sq,
        jnp.sum(start_part * lifted, axis=1, keepdims=True),
        jnp.sum(lifted * lifted, axis=1, keepdims=True),
        start_dot,
        jnp.sum(lifted * mix_weight, axis=1, keepdims=True),
    )
    lane = lax.broadcasted_iota(jnp.int32, (seqs, 128), 1)
    packed = jnp.zeros((seqs, 128), f32)
    for i, value in enumerate(sums):
        packed = packed + jnp.where(lane == i, value, 0.0)
    st_send[...] = packed
    stat_copies = tp_copies(1, lambda peer: st_send, st_recv.at[tp])
    arrive(stat_copies)
    for d in range(1, tp_count):
        packed = packed + st_recv[from_tp(d)]
    branch_sq, start_sq, cross_sum, lifted_sq, start_dot, lifted_dot = (
        packed[:, i : i + 1] for i in range(6)
    )
    branch_scale = lax.rsqrt(branch_sq / width + EPS)
    residual_f = start_part + lifted * branch_scale
    resid_sq = start_sq + 2.0 * branch_scale * cross_sum + branch_scale * branch_scale * lifted_sq
    gate_dot = start_dot + branch_scale * lifted_dot
    scale_two = lax.rsqrt(resid_sq / width + EPS)
    mix_gate = jax.nn.sigmoid(scale_two * gate_dot)
    residual = residual_f.astype(bf16).astype(f32)
    normed = (residual_f * scale_two * gain_two).astype(bf16)
    my_rows = pl.ds(pl.multiple_of(ep * seqs, seqs), seqs)
    rows_in[my_rows, :] = normed
    row_copies = ep_copies(1, lambda peer: rows_in.at[my_rows], rows_in.at[my_rows])

    arrive(code_copies)
    codes = code_send[...]
    for d in range(1, ep_count):
        codes = codes + code_recv[from_ep(d)]
    expert = lax.broadcasted_iota(jnp.int32, codes.shape, 0)
    mine = jnp.sum(jnp.where(expert == ep, codes, 0.0), axis=0, keepdims=True)
    slot = lax.broadcasted_iota(jnp.int32, (slots, rows_all), 0)
    token = lax.broadcasted_iota(jnp.int32, (slots, rows_all), 1)
    wanted = (lax.rem(slot, capacity) + 1).astype(f32)
    placing = jnp.where(
        jnp.logical_and(slot // capacity == token // seqs, mine == wanted), 1.0, 0.0
    ).astype(bf16)

    arrive(row_copies)
    rows = rows_in[...]
    xin[tp] = jnp.dot(placing, rows, preferred_element_type=f32).astype(bf16)
    def block_rows(peer):
        return pl.ds(pl.multiple_of(peer * rows_tp, rows_tp), rows_tp)

    def xin_at(i):
        return xin.at[i]

    def pre_at(i):
        return pre_send.at[:, block_rows(i)]

    def hid_at(i):
        return hid.at[block_rows(i)]

    def eo_at(i):
        return eo_send.at[i]

    expert_copies = gather_start(2, xin_at)

    loads[0].wait()
    loads[1].wait()
    last = (((1,), (1,)), ((), ()))
    pre_send[0] = lax.dot_general(rows, dg[...], last, preferred_element_type=f32).astype(bf16)
    pre_send[1] = lax.dot_general(rows, du[...], last, preferred_element_type=f32).astype(bf16)
    pre_copies = scatter_pair(3, pre_at, pre_one)

    loads[2].wait()
    loads[3].wait()
    gate_pre = jnp.dot(xin[tp], eg[columns(tp), :], preferred_element_type=f32)
    up_pre = jnp.dot(xin[tp], eu[columns(tp), :], preferred_element_type=f32)
    scatter_cross(3, pre_at, pre_one, pre_mid, pre_two, pre_copies)
    expert_copies[groups - 1].wait_recv()
    gate_pre = gate_pre + jnp.dot(xin[pair], eg[columns(pair), :], preferred_element_type=f32)
    up_pre = up_pre + jnp.dot(xin[pair], eu[columns(pair), :], preferred_element_type=f32)
    gather_relay(2, xin_at, expert_copies)
    for d in range(1, groups):
        source = behind(d)
        gate_pre = gate_pre + jnp.dot(xin[source], eg[columns(source), :], preferred_element_type=f32)
        up_pre = up_pre + jnp.dot(xin[source], eu[columns(source), :], preferred_element_type=f32)
    for d in range(1, groups):
        expert_copies[groups - 1 + d].wait_recv()
        source = behind(d) + 1 - 2 * parity
        gate_pre = gate_pre + jnp.dot(xin[source], eg[columns(source), :], preferred_element_type=f32)
        up_pre = up_pre + jnp.dot(xin[source], eu[columns(source), :], preferred_element_type=f32)
    hidden_units = (jax.nn.silu(gate_pre) * up_pre).astype(bf16)

    pre = scatter_sum(pre_at, pre_one, pre_two, pre_copies)
    hid[block_rows(tp), :] = (jax.nn.silu(pre[0]) * pre[1]).astype(bf16)
    hid_copies = gather_start(4, hid_at)

    loads[5].wait()
    for j in range(groups):
        t = j * 2 + 1 - parity
        eo_send[t] = jnp.dot(hidden_units, ed[:, columns(t)], preferred_element_type=f32).astype(bf16)
    eo_copies = scatter_pair(5, eo_at, eo_one)
    for j in range(groups):
        t = j * 2 + parity
        eo_send[t] = jnp.dot(hidden_units, ed[:, columns(t)], preferred_element_type=f32).astype(bf16)
    scatter_cross(5, eo_at, eo_one, eo_mid, eo_two, eo_copies)
    gather_relay(4, hid_at, hid_copies)
    for copy in hid_copies[groups - 1 :]:
        copy.wait_recv()
    loads[4].wait()
    down_send[...] = jnp.dot(hid[...], dd[...], preferred_element_type=f32).astype(bf16)

    def seq_rows(peer):
        return pl.ds(pl.multiple_of(peer * seqs, seqs), seqs)

    down_copies = ep_copies(2, lambda peer: down_send.at[seq_rows(peer)], down_recv.at[ep])

    total = scatter_sum(eo_at, eo_one, eo_two, eo_copies)
    sum_send[...] = total.astype(bf16)

    def slot_rows(peer):
        return pl.ds(pl.multiple_of(peer * capacity, capacity), capacity)

    back_copies = ep_copies(3, lambda peer: sum_send.at[slot_rows(peer)], returned.at[slot_rows(ep)])
    returned[slot_rows(ep), :] = sum_send[slot_rows(ep), :]

    arrive(down_copies)
    dense_out = down_send[seq_rows(ep), :].astype(f32)
    for d in range(1, ep_count):
        dense_out = dense_out + down_recv[from_ep(d)].astype(f32)
    ffn = mix_gate * dense_out
    arrive(back_copies)
    first_dims = (((0,), (0,)), ((), ()))
    for k in range(top):
        picked = lax.dot_general(combines[k], returned[...], first_dims, preferred_element_type=f32)
        ffn = ffn + shares[k] * picked
    squares = jnp.where(lane == 0, jnp.sum(ffn * ffn, axis=1, keepdims=True), 0.0)
    fs_send[...] = squares
    final_copies = tp_copies(6, lambda peer: fs_send, fs_recv.at[tp])
    scaled = gain_three * ffn
    arrive(final_copies)
    for d in range(1, tp_count):
        squares = squares + fs_recv[from_tp(d)]
    out_ref[...] = (residual + scaled * lax.rsqrt(squares[:, 0:1] / width + EPS)).astype(bf16)
    for copies in (
        branch_copies,
        code_copies,
        stat_copies,
        row_copies,
        expert_copies,
        pre_copies,
        hid_copies,
        eo_copies,
        down_copies,
        back_copies,
        final_copies,
    ):
        left(copies)


def tail(
    terms, hidden, norm_gains, dense_mix, routes, route_scores, weights
):
    tp_count = lax.axis_size("tp")
    ep_count = lax.axis_size("ep")
    seqs, width = hidden.shape
    part = width // tp_count
    expert_gate, expert_up, expert_down, dense_gate, dense_up, dense_down = weights
    units = expert_gate.shape[2]
    dense_gate, dense_up = dense_gate.T, dense_up.T
    dense_units = dense_gate.shape[0]
    top = routes.shape[1]
    experts = ep_count * expert_gate.shape[0]
    limit = 2 * seqs * top // ep_count
    capacity = -(-limit // 16) * 16
    rows_all = ep_count * seqs
    rows_tp = rows_all // tp_count
    groups = tp_count // 2
    f32, bf16 = jnp.float32, jnp.bfloat16
    vmem = pl.BlockSpec(memory_space=pltpu.VMEM)
    hbm = pl.BlockSpec(memory_space=pl.ANY)
    slots = ep_count * capacity
    return pl.pallas_call(
        functools.partial(tail_kernel, tp_count, ep_count, capacity),
        out_shape=jax.ShapeDtypeStruct((seqs, part), bf16),
        in_specs=[vmem] * 6 + [hbm] * 6,
        out_specs=vmem,
        scratch_shapes=[
            pltpu.VMEM((width, units), bf16),
            pltpu.VMEM((width, units), bf16),
            pltpu.VMEM((units, width), bf16),
            pltpu.VMEM(dense_gate.shape, bf16),
            pltpu.VMEM(dense_up.shape, bf16),
            pltpu.VMEM(dense_down.shape, bf16),
            pltpu.VMEM((tp_count, seqs, part), bf16),
            pltpu.VMEM((seqs, 128), f32),
            pltpu.VMEM((tp_count, seqs, 128), f32),
            pltpu.VMEM((seqs, 128), f32),
            pltpu.VMEM((tp_count, seqs, 128), f32),
            pltpu.VMEM((experts, rows_all), f32),
            pltpu.VMEM((ep_count, experts, rows_all), f32),
            pltpu.VMEM((rows_all, part), bf16),
            pltpu.VMEM((tp_count, slots, part), bf16),
            pltpu.VMEM((2, rows_all, dense_units), bf16),
            pltpu.VMEM((groups, 2, rows_tp, dense_units), bf16),
            pltpu.VMEM((groups, 2, rows_tp, dense_units), bf16),
            pltpu.VMEM((groups, 2, rows_tp, dense_units), bf16),
            pltpu.VMEM((rows_all, dense_units), bf16),
            pltpu.VMEM((rows_all, part), bf16),
            pltpu.VMEM((ep_count, seqs, part), bf16),
            pltpu.VMEM((tp_count, slots, part), bf16),
            pltpu.VMEM((groups, slots, part), bf16),
            pltpu.VMEM((groups, slots, part), bf16),
            pltpu.VMEM((groups, slots, part), bf16),
            pltpu.VMEM((slots, part), bf16),
            pltpu.VMEM((slots, part), bf16),
            pltpu.SemaphoreType.DMA((6,)),
            pltpu.SemaphoreType.DMA((7, tp_count - 1)),
            pltpu.SemaphoreType.DMA((7, tp_count - 1)),
            pltpu.SemaphoreType.DMA((4, ep_count - 1)),
            pltpu.SemaphoreType.DMA((4, ep_count - 1)),
        ],
        compiler_params=pltpu.CompilerParams(
            collective_id=0, has_side_effects=True, vmem_limit_bytes=56 * 1024 * 1024
        ),
        name="tail",
    )(
        terms,
        hidden,
        norm_gains,
        dense_mix.reshape(1, width),
        routes.T,
        route_scores.T,
        expert_gate,
        expert_up,
        expert_down,
        dense_gate,
        dense_up,
        dense_down,
    )


def local(
    hidden,
    norm_gains,
    w_query,
    w_key,
    w_value,
    w_outgate,
    w_input_gate,
    w_forget_gate,
    forget_bias,
    w_mix_out,
    state_matrix,
    state_norm,
    state_max,
    routes,
    route_scores,
    expert_gate,
    expert_up,
    expert_down,
    dense_gate,
    dense_up,
    dense_down,
    dense_mix,
):
    terms, new_matrix, new_norm, new_max = front(
        hidden,
        norm_gains,
        (w_input_gate, w_forget_gate),
        forget_bias,
        state_norm,
        state_max,
        (w_query, w_key, w_value, w_outgate, w_mix_out),
        state_matrix,
    )
    new_hidden = tail(
        terms,
        hidden,
        norm_gains,
        dense_mix,
        routes,
        route_scores,
        (expert_gate, expert_up, expert_down, dense_gate, dense_up, dense_down),
    )
    return (new_hidden, new_matrix, new_norm, new_max)


def solution(mesh):
    placed = (
        P("ep", None),
        P(),
        P(None, "tp"),
        P(None, "tp"),
        P(None, "tp"),
        P(None, "tp"),
        P(),
        P(),
        P(),
        P("tp", None),
        P("ep", "tp", None, None),
        P("ep", "tp", None),
        P("ep", "tp"),
        P("ep", None),
        P("ep", None),
        P("ep", None, "tp"),
        P("ep", None, "tp"),
        P("ep", "tp", None),
        P("tp", "ep"),
        P("tp", "ep"),
        P("ep", "tp"),
        P(),
    )
    return jax.shard_map(
        local,
        mesh=mesh,
        in_specs=placed,
        out_specs=(P("ep", "tp"), P("ep", "tp", None, None), P("ep", "tp", None), P("ep", "tp")),
        check_vma=False,
    )
```

```python
import functools

import jax
import jax.numpy as jnp
from jax import lax
from jax.experimental import pallas as pl
from jax.experimental.pallas import tpu as pltpu
from jax.sharding import PartitionSpec as P

EPS = 1e-06


def front_kernel(
    hidden_ref,
    gains_ref,
    in_ref,
    forget_ref,
    bias_ref,
    norm_ref,
    max_ref,
    wq_hbm,
    wk_hbm,
    wv_hbm,
    wo_hbm,
    wm_hbm,
    state_hbm,
    terms_ref,
    matrix_hbm,
    new_norm_ref,
    new_max_ref,
    wq,
    wk,
    wv,
    wo,
    wm,
    state,
    numer,
    w_sem,
    in_sem,
    out_sem,
):
    tp = lax.axis_index("tp")
    f32, bf16 = jnp.float32, jnp.bfloat16
    seqs = hidden_ref.shape[0]
    heads, head = state.shape[1], state.shape[2]
    chunks = in_sem.shape[0]
    step = seqs // chunks
    loads = []
    for i, (src, dst) in enumerate(((wk_hbm, wk), (wq_hbm, wq), (wv_hbm, wv), (wo_hbm, wo))):
        loads.append(pltpu.make_async_copy(src, dst, w_sem.at[i]))
        loads[i].start()
    fetches = []
    for c in range(chunks):
        rows = pl.ds(c * step, step)
        fetches.append(pltpu.make_async_copy(state_hbm.at[rows], state.at[rows], in_sem.at[c]))
        fetches[c].start()
    loads.append(pltpu.make_async_copy(wm_hbm, wm, w_sem.at[4]))
    loads[4].start()

    start = hidden_ref[...].astype(f32)
    scale = lax.rsqrt(jnp.mean(start * start, axis=1, keepdims=True) + EPS)
    normed = (start * scale * gains_ref[0:1, :]).astype(bf16)
    last = (((1,), (1,)), ((), ()))
    in_all = lax.dot_general(normed, in_ref[...], last, preferred_element_type=f32)
    forget_all = lax.dot_general(normed, forget_ref[...], last, preferred_element_type=f32)
    forget_all = forget_all + bias_ref[...]
    forget_all = jnp.minimum(forget_all, 0.0) - jnp.log(1.0 + jnp.exp(-jnp.abs(forget_all)))
    column = lax.broadcasted_iota(jnp.int32, in_all.shape, 1)
    here = lax.broadcasted_iota(jnp.int32, (seqs, seqs), 0)
    there = lax.broadcasted_iota(jnp.int32, (seqs, seqs), 1)
    projected = []
    for i, weight in enumerate((wk, wq, wv)):
        loads[i].wait()
        product = jnp.dot(normed, weight[...], preferred_element_type=f32)
        projected.append(product.astype(bf16).astype(f32))
    keys, query, values = projected
    pieces = []
    for h in range(heads):
        span = slice(h * head, (h + 1) * head)
        pieces.extend((keys[:, span], query[:, span]))
    turned = jnp.concatenate(pieces, axis=0).T
    keeps = []
    adds = []
    bounds = []
    for h in range(heads):
        span = slice(h * head, (h + 1) * head)
        mine = column == tp * heads + h
        in_gate = jnp.sum(jnp.where(mine, in_all, 0.0), axis=1, keepdims=True)
        log_forget = jnp.sum(jnp.where(mine, forget_all, 0.0), axis=1, keepdims=True)
        before = jnp.sum(jnp.where(here == there, max_ref[h : h + 1, :], 0.0), axis=1, keepdims=True)
        carried = log_forget + before
        new_max = jnp.maximum(carried, in_gate)
        keep = jnp.exp(carried - new_max)
        write = jnp.exp(in_gate - new_max) * head ** (-0.5)
        new_max_ref[h : h + 1, :] = jnp.sum(
            jnp.where(here == there, new_max, 0.0), axis=0, keepdims=True
        )
        new_norm = keep * norm_ref[:, h, :] + write * keys[:, span]
        new_norm_ref[:, h, :] = new_norm
        denom = jnp.sum(query[:, span] * new_norm, axis=1, keepdims=True)
        bounds.append(jnp.maximum(jnp.abs(denom), jnp.exp(-new_max)))
        keeps.append(jnp.broadcast_to(keep, (seqs, head)))
        adds.append(write * values[:, span])
    stores = []
    for c in range(chunks):
        fetches[c].wait()
        for s in range(c * step, (c + 1) * step):
            for h in range(heads):
                at = 2 * h * seqs + s
                key_col = turned[:, at : at + 1]
                query_col = turned[:, at + seqs : at + seqs + 1]
                new = keeps[h][s : s + 1, :] * state[s, h] + key_col * adds[h][s : s + 1, :]
                state[s, h] = new
                numer[h, s : s + 1, :] = jnp.sum(query_col * new, axis=0, keepdims=True)
        rows = pl.ds(c * step, step)
        stores.append(pltpu.make_async_copy(state.at[rows], matrix_hbm.at[rows], out_sem.at[c]))
        stores[c].start()
    loads[3].wait()
    gate = jnp.dot(normed, wo[...], preferred_element_type=f32).astype(bf16).astype(f32)
    mixed = []
    for h in range(heads):
        span = slice(h * head, (h + 1) * head)
        mixed.append((jax.nn.sigmoid(gate[:, span]) * (numer[h] / bounds[h])).astype(bf16))
    mixed = jnp.concatenate(mixed, axis=1)
    loads[4].wait()
    part = terms_ref.shape[2]
    for t in range(terms_ref.shape[0]):
        terms_ref[t] = jnp.dot(
            mixed, wm[:, t * part : (t + 1) * part], preferred_element_type=f32
        ).astype(bf16)
    for store in stores:
        store.wait()


def front(hidden, norm_gains, gate_weights, forget_bias, state_norm, state_max, weights, state_matrix):
    tp_count = lax.axis_size("tp")
    seqs, width = hidden.shape
    heads, head = state_matrix.shape[1], state_matrix.shape[2]
    f32, bf16 = jnp.float32, jnp.bfloat16
    chunks = 4
    vmem = pl.BlockSpec(memory_space=pltpu.VMEM)
    hbm = pl.BlockSpec(memory_space=pl.ANY)
    terms, matrix, norm, top = pl.pallas_call(
        front_kernel,
        out_shape=(
            jax.ShapeDtypeStruct((tp_count, seqs, width // tp_count), bf16),
            jax.ShapeDtypeStruct(state_matrix.shape, f32),
            jax.ShapeDtypeStruct(state_norm.shape, f32),
            jax.ShapeDtypeStruct((heads, seqs), f32),
        ),
        in_specs=[vmem] * 7 + [hbm] * 6,
        out_specs=(vmem, hbm, vmem, vmem),
        scratch_shapes=[pltpu.VMEM(weight.shape, bf16) for weight in weights]
        + [
            pltpu.VMEM(state_matrix.shape, f32),
            pltpu.VMEM((heads, seqs, head), f32),
            pltpu.SemaphoreType.DMA((5,)),
            pltpu.SemaphoreType.DMA((chunks,)),
            pltpu.SemaphoreType.DMA((chunks,)),
        ],
        compiler_params=pltpu.CompilerParams(vmem_limit_bytes=67043328),
        name="front",
    )(
        hidden,
        norm_gains,
        gate_weights[0].T,
        gate_weights[1].T,
        forget_bias.reshape(1, -1),
        state_norm,
        state_max.T,
        *weights,
        state_matrix,
    )
    return terms, matrix, norm, top.T


MESH = pl.DeviceIdType.MESH


def tail_kernel(
    tp_count,
    ep_count,
    capacity,
    terms_ref,
    hidden_ref,
    gains_ref,
    mix_ref,
    routes_ref,
    scores_ref,
    eg_hbm,
    eu_hbm,
    ed_hbm,
    dg_hbm,
    du_hbm,
    dd_hbm,
    out_ref,
    eg,
    eu,
    ed,
    dg,
    du,
    dd,
    br_recv,
    st_send,
    st_recv,
    fs_send,
    fs_recv,
    code_send,
    code_recv,
    rows_in,
    xin,
    pre_send,
    pre_one,
    pre_mid,
    pre_two,
    hid,
    down_send,
    down_recv,
    eo_send,
    eo_one,
    eo_mid,
    eo_two,
    sum_send,
    returned,
    w_sem,
    tp_send,
    tp_recv,
    ep_send,
    ep_recv,
):
    tp = lax.axis_index("tp")
    ep = lax.axis_index("ep")
    seqs, width = hidden_ref.shape
    part = width // tp_count
    rows_all = ep_count * seqs
    rows_tp = rows_all // tp_count
    first = pl.multiple_of(tp * part, part)
    f32, bf16 = jnp.float32, jnp.bfloat16

    loads = []
    for i, (src, dst) in enumerate(
        ((dg_hbm, dg), (du_hbm, du), (eg_hbm.at[0], eg), (eu_hbm.at[0], eu), (dd_hbm, dd), (ed_hbm.at[0], ed))
    ):
        load = pltpu.make_async_copy(src, dst, w_sem.at[i])
        load.start()
        loads.append(load)

    barrier = pltpu.get_barrier_semaphore()
    for d in range(1, tp_count):
        pl.semaphore_signal(
            barrier, inc=1, device_id={"tp": lax.rem(tp + d, tp_count)}, device_id_type=MESH
        )
    for d in range(1, ep_count):
        pl.semaphore_signal(
            barrier, inc=1, device_id={"ep": lax.rem(ep + d, ep_count)}, device_id_type=MESH
        )
    pl.semaphore_wait(barrier, tp_count - 1 + ep_count - 1)

    def tp_copies(phase, src_of, dst):
        made = []
        for d in range(1, tp_count):
            peer = lax.rem(tp + d, tp_count)
            copy = pltpu.make_async_remote_copy(
                src_ref=src_of(peer),
                dst_ref=dst,
                send_sem=tp_send.at[phase, d - 1],
                recv_sem=tp_recv.at[phase, d - 1],
                device_id={"tp": peer},
                device_id_type=MESH,
            )
            copy.start()
            made.append(copy)
        return made

    groups = tp_count // 2
    parity = lax.rem(tp, 2)
    group = tp // 2
    pair = tp + 1 - 2 * parity

    def one_copy(phase, i, src, dst, peer):
        copy = pltpu.make_async_remote_copy(
            src_ref=src,
            dst_ref=dst,
            send_sem=tp_send.at[phase, i],
            recv_sem=tp_recv.at[phase, i],
            device_id={"tp": peer},
            device_id_type=MESH,
        )
        copy.start()
        return copy

    def ahead(d):
        return lax.rem(group + d, groups) * 2 + parity

    def behind(d):
        return lax.rem(group + groups - d, groups) * 2 + parity

    def gather_start(phase, at):
        made = [one_copy(phase, d - 1, at(tp), at(tp), ahead(d)) for d in range(1, groups)]
        made.append(one_copy(phase, groups - 1, at(tp), at(tp), pair))
        return made

    def gather_relay(phase, at, made):
        for d in range(1, groups):
            made[d - 1].wait_recv()
            made.append(one_copy(phase, groups - 1 + d, at(behind(d)), at(behind(d)), pair))

    def scatter_pair(phase, at, one):
        return [
            one_copy(phase, j, at(j * 2 + 1 - parity), one.at[j], pair) for j in range(groups)
        ]

    def scatter_cross(phase, at, one, mid, two, made):
        arrive(made)
        for d in range(1, groups):
            j = lax.rem(group + d, groups)
            mid[j] = (at(ahead(d))[...].astype(f32) + one[j].astype(f32)).astype(bf16)
            made.append(one_copy(phase, groups + d - 1, mid.at[j], two.at[group], ahead(d)))

    def scatter_sum(at, one, two, made):
        total = at(tp)[...].astype(f32) + one[group].astype(f32)
        for d in range(1, groups):
            made[groups + d - 1].wait_recv()
            total = total + two[lax.rem(group + groups - d, groups)].astype(f32)
        return total

    def ep_copies(phase, src_of, dst):
        made = []
        for d in range(1, ep_count):
            peer = lax.rem(ep + d, ep_count)
            copy = pltpu.make_async_remote_copy(
                src_ref=src_of(peer),
                dst_ref=dst,
                send_sem=ep_send.at[phase, d - 1],
                recv_sem=ep_recv.at[phase, d - 1],
                device_id={"ep": peer},
                device_id_type=MESH,
            )
            copy.start()
            made.append(copy)
        return made

    def arrive(copies):
        for copy in copies:
            copy.wait_recv()

    def left(copies):
        for copy in copies:
            copy.wait_send()

    def from_tp(d):
        return lax.rem(tp + tp_count - d, tp_count)

    def from_ep(d):
        return lax.rem(ep + ep_count - d, ep_count)

    def columns(peer):
        return pl.ds(pl.multiple_of(peer * part, part), part)

    branch_copies = tp_copies(0, lambda peer: terms_ref.at[peer], br_recv.at[tp])
    top = routes_ref.shape[0]
    experts = code_send.shape[0]
    name = lax.broadcasted_iota(jnp.int32, (experts, seqs), 0)
    hits = [routes_ref[k : k + 1, :] == name for k in range(top)]
    named = hits[0]
    for k in range(1, top):
        named = jnp.logical_or(named, hits[k])
    named = jnp.where(named, 1.0, 0.0)
    here = lax.broadcasted_iota(jnp.int32, (seqs, seqs), 0)
    there = lax.broadcasted_iota(jnp.int32, (seqs, seqs), 1)
    before = jnp.where(here < there, 1.0, 0.0).astype(bf16)
    rank = jnp.dot(named.astype(bf16), before, preferred_element_type=f32) + 1.0
    code = (named * rank).astype(bf16)
    from_row = lax.broadcasted_iota(jnp.int32, (seqs, rows_all), 0)
    to_row = lax.broadcasted_iota(jnp.int32, (seqs, rows_all), 1)
    spread = jnp.where(from_row + ep * seqs == to_row, 1.0, 0.0).astype(bf16)
    code_send[...] = jnp.dot(code, spread, preferred_element_type=f32)
    code_copies = ep_copies(0, lambda peer: code_send, code_recv.at[ep])
    slots = ep_count * capacity
    owner = lax.broadcasted_iota(jnp.int32, (slots, experts), 0) // capacity
    of_expert = lax.broadcasted_iota(jnp.int32, (slots, experts), 1)
    widen = jnp.where(owner == of_expert, 1.0, 0.0).astype(bf16)
    row_slot = lax.broadcasted_iota(jnp.int32, (slots, seqs), 0)
    row_wanted = (lax.rem(row_slot, capacity) + 1).astype(f32)
    combines = []
    shares = []
    score_sum = scores_ref[0:1, :]
    for k in range(1, top):
        score_sum = score_sum + scores_ref[k : k + 1, :]
    for k in range(top):
        code_k = jnp.where(hits[k], rank, 0.0).astype(bf16)
        wide = jnp.dot(widen, code_k, preferred_element_type=f32)
        combines.append(jnp.where(wide == row_wanted, 1.0, 0.0).astype(bf16))
        share = scores_ref[k : k + 1, :] / score_sum
        shares.append(jnp.sum(jnp.where(here == there, share, 0.0), axis=1, keepdims=True))
    start_part = hidden_ref[:, pl.ds(first, part)].astype(f32)
    gain_one = gains_ref[1:2, pl.ds(first, part)]
    gain_two = gains_ref[2:3, pl.ds(first, part)]
    gain_three = gains_ref[3:4, pl.ds(first, part)]
    mix_weight = gain_two * mix_ref[:, pl.ds(first, part)]
    start_sq = jnp.sum(start_part * start_part, axis=1, keepdims=True)
    start_dot = jnp.sum(start_part * mix_weight, axis=1, keepdims=True)
    branch = terms_ref[tp].astype(f32)
    arrive(branch_copies)
    for d in range(1, tp_count):
        branch = branch + br_recv[from_tp(d)].astype(f32)
    branch = branch.astype(bf16).astype(f32)
    lifted = gain_one * branch
    sums = (
        jnp.sum(branch * branch, axis=1, keepdims=True),
        start_sq,
        jnp.sum(start_part * lifted, axis=1, keepdims=True),
        jnp.sum(lifted * lifted, axis=1, keepdims=True),
        start_dot,
        jnp.sum(lifted * mix_weight, axis=1, keepdims=True),
    )
    lane = lax.broadcasted_iota(jnp.int32, (seqs, 128), 1)
    packed = jnp.zeros((seqs, 128), f32)
    for i, value in enumerate(sums):
        packed = packed + jnp.where(lane == i, value, 0.0)
    st_send[...] = packed
    stat_copies = tp_copies(1, lambda peer: st_send, st_recv.at[tp])
    arrive(stat_copies)
    for d in range(1, tp_count):
        packed = packed + st_recv[from_tp(d)]
    branch_sq, start_sq, cross_sum, lifted_sq, start_dot, lifted_dot = (
        packed[:, i : i + 1] for i in range(6)
    )
    branch_scale = lax.rsqrt(branch_sq / width + EPS)
    residual_f = start_part + lifted * branch_scale
    resid_sq = start_sq + 2.0 * branch_scale * cross_sum + branch_scale * branch_scale * lifted_sq
    gate_dot = start_dot + branch_scale * lifted_dot
    scale_two = lax.rsqrt(resid_sq / width + EPS)
    mix_gate = jax.nn.sigmoid(scale_two * gate_dot)
    residual = residual_f.astype(bf16).astype(f32)
    normed = (residual_f * scale_two * gain_two).astype(bf16)
    my_rows = pl.ds(pl.multiple_of(ep * seqs, seqs), seqs)
    rows_in[my_rows, :] = normed
    row_copies = ep_copies(1, lambda peer: rows_in.at[my_rows], rows_in.at[my_rows])

    arrive(code_copies)
    codes = code_send[...]
    for d in range(1, ep_count):
        codes = codes + code_recv[from_ep(d)]
    expert = lax.broadcasted_iota(jnp.int32, codes.shape, 0)
    mine = jnp.sum(jnp.where(expert == ep, codes, 0.0), axis=0, keepdims=True)
    slot = lax.broadcasted_iota(jnp.int32, (slots, rows_all), 0)
    token = lax.broadcasted_iota(jnp.int32, (slots, rows_all), 1)
    wanted = (lax.rem(slot, capacity) + 1).astype(f32)
    placing = jnp.where(
        jnp.logical_and(slot // capacity == token // seqs, mine == wanted), 1.0, 0.0
    ).astype(bf16)

    arrive(row_copies)
    rows = rows_in[...]
    xin[tp] = jnp.dot(placing, rows, preferred_element_type=f32).astype(bf16)
    def block_rows(peer):
        return pl.ds(pl.multiple_of(peer * rows_tp, rows_tp), rows_tp)

    def xin_at(i):
        return xin.at[i]

    def pre_at(i):
        return pre_send.at[:, block_rows(i)]

    def hid_at(i):
        return hid.at[block_rows(i)]

    def eo_at(i):
        return eo_send.at[i]

    expert_copies = gather_start(2, xin_at)

    loads[0].wait()
    loads[1].wait()
    last = (((1,), (1,)), ((), ()))
    pre_send[0] = lax.dot_general(rows, dg[...], last, preferred_element_type=f32).astype(bf16)
    pre_send[1] = lax.dot_general(rows, du[...], last, preferred_element_type=f32).astype(bf16)
    pre_copies = scatter_pair(3, pre_at, pre_one)

    loads[2].wait()
    loads[3].wait()
    gate_pre = jnp.dot(xin[tp], eg[columns(tp), :], preferred_element_type=f32)
    up_pre = jnp.dot(xin[tp], eu[columns(tp), :], preferred_element_type=f32)
    scatter_cross(3, pre_at, pre_one, pre_mid, pre_two, pre_copies)
    expert_copies[groups - 1].wait_recv()
    gate_pre = gate_pre + jnp.dot(xin[pair], eg[columns(pair), :], preferred_element_type=f32)
    up_pre = up_pre + jnp.dot(xin[pair], eu[columns(pair), :], preferred_element_type=f32)
    gather_relay(2, xin_at, expert_copies)
    for d in range(1, groups):
        source = behind(d)
        gate_pre = gate_pre + jnp.dot(xin[source], eg[columns(source), :], preferred_element_type=f32)
        up_pre = up_pre + jnp.dot(xin[source], eu[columns(source), :], preferred_element_type=f32)
    for d in range(1, groups):
        expert_copies[groups - 1 + d].wait_recv()
        source = behind(d) + 1 - 2 * parity
        gate_pre = gate_pre + jnp.dot(xin[source], eg[columns(source), :], preferred_element_type=f32)
        up_pre = up_pre + jnp.dot(xin[source], eu[columns(source), :], preferred_element_type=f32)
    hidden_units = (jax.nn.silu(gate_pre) * up_pre).astype(bf16)

    pre = scatter_sum(pre_at, pre_one, pre_two, pre_copies)
    hid[block_rows(tp), :] = (jax.nn.silu(pre[0]) * pre[1]).astype(bf16)
    hid_copies = gather_start(4, hid_at)

    loads[5].wait()
    for j in range(groups):
        t = j * 2 + 1 - parity
        eo_send[t] = jnp.dot(hidden_units, ed[:, columns(t)], preferred_element_type=f32).astype(bf16)
    eo_copies = scatter_pair(5, eo_at, eo_one)
    for j in range(groups):
        t = j * 2 + parity
        eo_send[t] = jnp.dot(hidden_units, ed[:, columns(t)], preferred_element_type=f32).astype(bf16)
    scatter_cross(5, eo_at, eo_one, eo_mid, eo_two, eo_copies)
    gather_relay(4, hid_at, hid_copies)
    for copy in hid_copies[groups - 1 :]:
        copy.wait_recv()
    loads[4].wait()
    down_send[...] = jnp.dot(hid[...], dd[...], preferred_element_type=f32).astype(bf16)

    def seq_rows(peer):
        return pl.ds(pl.multiple_of(peer * seqs, seqs), seqs)

    down_copies = ep_copies(2, lambda peer: down_send.at[seq_rows(peer)], down_recv.at[ep])

    total = scatter_sum(eo_at, eo_one, eo_two, eo_copies)
    sum_send[...] = total.astype(bf16)

    def slot_rows(peer):
        return pl.ds(pl.multiple_of(peer * capacity, capacity), capacity)

    back_copies = ep_copies(3, lambda peer: sum_send.at[slot_rows(peer)], returned.at[slot_rows(ep)])
    returned[slot_rows(ep), :] = sum_send[slot_rows(ep), :]

    arrive(down_copies)
    dense_out = down_send[seq_rows(ep), :].astype(f32)
    for d in range(1, ep_count):
        dense_out = dense_out + down_recv[from_ep(d)].astype(f32)
    ffn = mix_gate * dense_out
    arrive(back_copies)
    first_dims = (((0,), (0,)), ((), ()))
    for k in range(top):
        picked = lax.dot_general(combines[k], returned[...], first_dims, preferred_element_type=f32)
        ffn = ffn + shares[k] * picked
    squares = jnp.where(lane == 0, jnp.sum(ffn * ffn, axis=1, keepdims=True), 0.0)
    fs_send[...] = squares
    final_copies = tp_copies(6, lambda peer: fs_send, fs_recv.at[tp])
    scaled = gain_three * ffn
    arrive(final_copies)
    for d in range(1, tp_count):
        squares = squares + fs_recv[from_tp(d)]
    out_ref[...] = (residual + scaled * lax.rsqrt(squares[:, 0:1] / width + EPS)).astype(bf16)
    for copies in (
        branch_copies,
        code_copies,
        stat_copies,
        row_copies,
        expert_copies,
        pre_copies,
        hid_copies,
        eo_copies,
        down_copies,
        back_copies,
        final_copies,
    ):
        left(copies)


def tail(
    terms, hidden, norm_gains, dense_mix, routes, route_scores, weights
):
    tp_count = lax.axis_size("tp")
    ep_count = lax.axis_size("ep")
    seqs, width = hidden.shape
    part = width // tp_count
    expert_gate, expert_up, expert_down, dense_gate, dense_up, dense_down = weights
    units = expert_gate.shape[2]
    dense_gate, dense_up = dense_gate.T, dense_up.T
    dense_units = dense_gate.shape[0]
    top = routes.shape[1]
    experts = ep_count * expert_gate.shape[0]
    limit = 2 * seqs * top // ep_count
    capacity = -(-limit // 16) * 16
    rows_all = ep_count * seqs
    rows_tp = rows_all // tp_count
    groups = tp_count // 2
    f32, bf16 = jnp.float32, jnp.bfloat16
    vmem = pl.BlockSpec(memory_space=pltpu.VMEM)
    hbm = pl.BlockSpec(memory_space=pl.ANY)
    slots = ep_count * capacity
    return pl.pallas_call(
        functools.partial(tail_kernel, tp_count, ep_count, capacity),
        out_shape=jax.ShapeDtypeStruct((seqs, part), bf16),
        in_specs=[vmem] * 6 + [hbm] * 6,
        out_specs=vmem,
        scratch_shapes=[
            pltpu.VMEM((width, units), bf16),
            pltpu.VMEM((width, units), bf16),
            pltpu.VMEM((units, width), bf16),
            pltpu.VMEM(dense_gate.shape, bf16),
            pltpu.VMEM(dense_up.shape, bf16),
            pltpu.VMEM(dense_down.shape, bf16),
            pltpu.VMEM((tp_count, seqs, part), bf16),
            pltpu.VMEM((seqs, 128), f32),
            pltpu.VMEM((tp_count, seqs, 128), f32),
            pltpu.VMEM((seqs, 128), f32),
            pltpu.VMEM((tp_count, seqs, 128), f32),
            pltpu.VMEM((experts, rows_all), f32),
            pltpu.VMEM((ep_count, experts, rows_all), f32),
            pltpu.VMEM((rows_all, part), bf16),
            pltpu.VMEM((tp_count, slots, part), bf16),
            pltpu.VMEM((2, rows_all, dense_units), bf16),
            pltpu.VMEM((groups, 2, rows_tp, dense_units), bf16),
            pltpu.VMEM((groups, 2, rows_tp, dense_units), bf16),
            pltpu.VMEM((groups, 2, rows_tp, dense_units), bf16),
            pltpu.VMEM((rows_all, dense_units), bf16),
            pltpu.VMEM((rows_all, part), bf16),
            pltpu.VMEM((ep_count, seqs, part), bf16),
            pltpu.VMEM((tp_count, slots, part), bf16),
            pltpu.VMEM((groups, slots, part), bf16),
            pltpu.VMEM((groups, slots, part), bf16),
            pltpu.VMEM((groups, slots, part), bf16),
            pltpu.VMEM((slots, part), bf16),
            pltpu.VMEM((slots, part), bf16),
            pltpu.SemaphoreType.DMA((6,)),
            pltpu.SemaphoreType.DMA((7, tp_count - 1)),
            pltpu.SemaphoreType.DMA((7, tp_count - 1)),
            pltpu.SemaphoreType.DMA((4, ep_count - 1)),
            pltpu.SemaphoreType.DMA((4, ep_count - 1)),
        ],
        compiler_params=pltpu.CompilerParams(
            collective_id=0, has_side_effects=True, vmem_limit_bytes=67043328
        ),
        name="tail",
    )(
        terms,
        hidden,
        norm_gains,
        dense_mix.reshape(1, width),
        routes.T,
        route_scores.T,
        expert_gate,
        expert_up,
        expert_down,
        dense_gate,
        dense_up,
        dense_down,
    )


def local(
    hidden,
    norm_gains,
    w_query,
    w_key,
    w_value,
    w_outgate,
    w_input_gate,
    w_forget_gate,
    forget_bias,
    w_mix_out,
    state_matrix,
    state_norm,
    state_max,
    routes,
    route_scores,
    expert_gate,
    expert_up,
    expert_down,
    dense_gate,
    dense_up,
    dense_down,
    dense_mix,
):
    terms, new_matrix, new_norm, new_max = front(
        hidden,
        norm_gains,
        (w_input_gate, w_forget_gate),
        forget_bias,
        state_norm,
        state_max,
        (w_query, w_key, w_value, w_outgate, w_mix_out),
        state_matrix,
    )
    new_hidden = tail(
        terms,
        hidden,
        norm_gains,
        dense_mix,
        routes,
        route_scores,
        (expert_gate, expert_up, expert_down, dense_gate, dense_up, dense_down),
    )
    return (new_hidden, new_matrix, new_norm, new_max)


def solution(mesh):
    placed = (
        P("ep", None),
        P(),
        P(None, "tp"),
        P(None, "tp"),
        P(None, "tp"),
        P(None, "tp"),
        P(),
        P(),
        P(),
        P("tp", None),
        P("ep", "tp", None, None),
        P("ep", "tp", None),
        P("ep", "tp"),
        P("ep", None),
        P("ep", None),
        P("ep", None, "tp"),
        P("ep", None, "tp"),
        P("ep", "tp", None),
        P("tp", "ep"),
        P("tp", "ep"),
        P("ep", "tp"),
        P(),
    )
    return jax.shard_map(
        local,
        mesh=mesh,
        in_specs=placed,
        out_specs=(P("ep", "tp"), P("ep", "tp", None, None), P("ep", "tp", None), P("ep", "tp")),
        check_vma=False,
    )
```
